32 devices in a mesh: fs: 8 (over z, y), tp: 4 (over x, core).
Axes of the slice: x: 2, y: 2, z: 4, core: 2. Of those that a mesh axis runs over, the one named last changes fastest.
Arguments:
- tokens: bfloat16 [6144, 2048], P('fs'), may hold values from -6 to 6
- routes: int32 [6144, 2], P('fs'), may hold values from 0 to 7, all different within a row; in each aligned block of 768 rows (0 to 767, 768 to 1535, ...) at most 216 rows name the same one
- route_weight: float32 [6144, 2], P('fs'), may hold values from 0.2 to 1
- norm_gain: float32 [2048], P('fs'), may hold values from 0.1 to 1.9
- gate_master: float32 [8, 2048, 4096], P(None, 'fs', 'tp'), may hold values from -0.125 to 0.125
- up_master: float32 [8, 2048, 4096], P(None, 'fs', 'tp'), may hold values from -0.125 to 0.125
- down_master: float32 [8, 4096, 2048], P(None, 'fs', 'tp'), may hold values from -0.09375 to 0.09375
Outputs:
- gate_serve: bfloat16 [8, 2048, 4096], P('fs', None, 'tp')
- up_serve: bfloat16 [8, 2048, 4096], P('fs', None, 'tp')
- down_serve: bfloat16 [8, 4096, 2048], P('fs', 'tp')
- layer_out: bfloat16 [6144, 2048], P('fs', 'tp')
The draws below stay inside these ranges and needn't reach their ends.
Inputs may be any that keep to these rules, and one draw needn't show every extreme that they name: `routes`: each row names two different experts; among the 768 rows of one index of fs no expert is named by more than 216 rows, a bound that some block reaches.
All inputs are finite; a program needn't handle non-finite values.
Results may differ from the reference program's by a relative error of at most 0.015.
Values may be sent and summed in bfloat16 or wider, within the bound.
A program may use at most 192 MiB of HBM per device.

```python
import math
import jax
import jax.numpy as jnp
import numpy as np
from jax import lax

D = 2048
FF = 4096
TOK_DEV = 768
CAP = 216
EXPERTS = 8
TOKENS = 6144
N_FS = 8
N_TP = 4


def block_scale(key, extent, shards, low, largest):
    loudness, own = 1.0, jax.random.fold_in(key, 6)
    for axis_at, parts in shards:
        draws = jnp.exp(jax.random.uniform(jax.random.fold_in(own, axis_at), (parts,), jnp.float32, low / len(shards), largest / len(shards)))
        loudness = loudness * jnp.repeat(draws, extent[axis_at] // parts).reshape([-1 if axis == axis_at else 1 for axis in range(len(extent))])
    return loudness


def deal_out(key, own, number, rows, count, top, reach, slope):
    order = jax.random.permutation(key, count)
    crowded, usual = portions_of(count, rows * top, reach, slope, True), portions_of(count, rows * top, reach, slope, False)
    places = jnp.arange(count)

    def named(lengths, turn):
        used = int((lengths > 0).sum())
        fixed = max(1, used // 4)
        passed = fixed + (places - fixed + turn * (used - fixed)) % max(1, count - fixed)
        return jnp.zeros((count,), jnp.int32).at[order[jnp.where(places < fixed, places, passed)]].set(jnp.asarray(lengths, jnp.int32))

    lengths = jnp.where(number % 4 == 0, named(crowded, number // 4), named(usual, number - number // 4 - 1))
    mixed = jax.random.permutation(jax.random.fold_in(own, 3), count)
    donor, sink = mixed[0:count // 2 * 2:2], mixed[1:count // 2 * 2:2]
    margin = jnp.minimum(lengths[donor] - 1, reach - lengths[sink]) // 2
    margin = jnp.where((donor == order[0]) | (sink == order[0]) | (lengths[sink] == 0), 0, jnp.maximum(margin, 0))
    passed = jax.random.randint(jax.random.fold_in(own, 4), (count // 2,), 0, 1 << 20) % (margin + 1)
    lengths = lengths.at[donor].add(-passed).at[sink].add(passed)
    labels = jnp.searchsorted(jnp.cumsum(lengths), jnp.arange(rows * top), side="right").astype(jnp.int32)
    table = labels.reshape(top, rows).T
    table = table[jax.random.permutation(jax.random.fold_in(own, 1), rows)]
    turn = jax.random.randint(jax.random.fold_in(own, 2), (rows, 1), 0, top)
    return jnp.take_along_axis(table, (jnp.arange(top)[None, :] + turn) % top, axis=1)


def portions_of(count, total, reach, slope, full):
    weights = [(1 << 20) // math.isqrt(rank ** slope) + 1 for rank in range(1, count + 1)]
    largest = reach if full else min(reach, max(-(-total // count), total * weights[0] // sum(weights)))
    least = 1 if total - largest >= count - 1 else 0
    holding, rest = [largest] + [least] * (count - 1), total - largest - least * (count - 1)
    while rest > 0:
        movable = [i for i in range(1, count) if holding[i] < largest] or [i for i in range(1, count) if holding[i] < reach]
        pool, remaining = sum([weights[i] for i in movable]), rest
        for i in movable:
            extra = min(reach - holding[i], max(1, remaining * weights[i] // pool), rest)
            holding[i] = holding[i] + extra
            rest = rest - extra
    return np.array(holding)


def centred(own_key, dims, deviation, most, pieces=(), kind=jnp.bfloat16):
    result = deviation * jax.random.normal(own_key, dims, jnp.float32)
    if pieces:
        result = result * block_scale(own_key, dims, pieces, -0.22, 0.18)
    return jnp.clip(result, -most, most).astype(kind)


def setup_inputs(seed: int = 0) -> dict:
    key_of = jax.random.split(jax.random.key(seed), 8)
    tokens = centred(key_of[0], (TOKENS, D), 1.0, 6.0, ((0, 8),))
    routes_keys = jax.random.split(jax.random.fold_in(key_of[1], 1), TOKENS // TOK_DEV)
    routes_turns = jax.random.permutation(jax.random.fold_in(key_of[1], 3), TOKENS // TOK_DEV)
    routes = jax.vmap(lambda own, number: deal_out(jax.random.fold_in(key_of[1], 2), own, number, TOK_DEV, EXPERTS, 2, CAP, 2))(routes_keys, routes_turns).reshape((TOKENS, 2))
    route_weight = jnp.clip(0.2 + 0.8 * jax.random.uniform(key_of[2], (TOKENS, 2), jnp.float32) ** block_scale(key_of[2], (TOKENS, 2), ((0, 8),), -0.2, 0.2), 0.2, 1.0)
    norm_gain = jnp.clip(1.0 + 0.18 * jax.random.normal(key_of[3], (D,), jnp.float32), 0.1, 1.9)
    gate_master = centred(key_of[4], (EXPERTS, D, FF), D ** -0.5, 0.125, ((1, 8), (2, 4)), jnp.float32)
    up_master = centred(key_of[5], (EXPERTS, D, FF), D ** -0.5, 0.125, ((1, 8), (2, 4)), jnp.float32)
    down_master = centred(key_of[6], (EXPERTS, FF, D), FF ** -0.5, 0.09375, ((1, 8), (2, 4)), jnp.float32)
    return dict(tokens=tokens, routes=routes, route_weight=route_weight, norm_gain=norm_gain, gate_master=gate_master, up_master=up_master, down_master=down_master)


def reference(tokens, routes, route_weight, norm_gain, gate_master, up_master, down_master):
    values = tokens.astype(jnp.float32)
    normed = (values * lax.rsqrt(lax.optimization_barrier(jnp.mean(values * values, axis=-1, keepdims=True)) + 1e-06)).astype(jnp.bfloat16)
    gate_serve = (norm_gain[None, :, None] * gate_master).astype(jnp.bfloat16)
    up_serve = (norm_gain[None, :, None] * up_master).astype(jnp.bfloat16)
    down_serve = down_master.astype(jnp.bfloat16)
    rows_cap = N_FS * CAP
    group_units = FF // N_TP

    def expert_step(totals, expert):
        is_routed = jnp.any(routes == expert, axis=1)
        ordering = jnp.argsort(jnp.where(is_routed, 0, 1).astype(jnp.int32), stable=True)[:rows_cap]
        present = is_routed[ordering]
        chosen_rows = jnp.where(present[:, None], normed[ordering], jnp.zeros((), jnp.bfloat16))
        gate_pre = jnp.dot(chosen_rows, gate_serve[expert], preferred_element_type=jnp.float32)
        up_pre = jnp.dot(chosen_rows, up_serve[expert], preferred_element_type=jnp.float32)
        hidden = (jax.nn.silu(gate_pre) * up_pre).astype(jnp.bfloat16)
        block_sums = jnp.einsum('rgf,gfd->grd', hidden.reshape(rows_cap, N_TP, group_units).astype(jnp.float32), down_serve[expert].reshape(N_TP, group_units, D).astype(jnp.float32))
        rounded = lax.optimization_barrier(block_sums.astype(jnp.bfloat16)).astype(jnp.float32)
        expert_out = lax.optimization_barrier(jnp.sum(rounded, axis=0)).astype(jnp.bfloat16)
        row_weight = lax.optimization_barrier(jnp.sum(jnp.where(routes[ordering] == expert, route_weight[ordering], jnp.zeros((), jnp.float32)), axis=1))
        row_weight = jnp.where(present, row_weight, jnp.zeros((), jnp.float32))
        totals = totals.at[ordering].add(row_weight[:, None] * expert_out.astype(jnp.float32))
        return (totals, None)
    totals, _ = lax.scan(expert_step, jnp.zeros((TOKENS, D), jnp.float32), jnp.arange(EXPERTS, dtype=jnp.int32))
    return (gate_serve, up_serve, down_serve, totals.astype(jnp.bfloat16))
```

```python
import jax
import jax.numpy as jnp
from jax import lax
from jax.experimental import pallas as pl
from jax.sharding import PartitionSpec as P


CAP = 216
CHUNKS = 2


def copy_kernel(source, target):
    target[...] = source[...]


def settled(value):
    rows, columns = value.shape
    spec = pl.BlockSpec((rows // 8, columns), lambda i: (i, 0))
    return pl.pallas_call(
        copy_kernel,
        grid=(8,),
        out_shape=jax.ShapeDtypeStruct(value.shape, value.dtype),
        in_specs=[spec],
        out_specs=spec,
        cost_estimate=pl.CostEstimate(
            flops=0, bytes_accessed=2 * value.size * value.dtype.itemsize, transcendentals=0
        ),
    )(value)


def added(kept, got):
    return [
        (k.astype(jnp.float32) + g.astype(jnp.float32)).astype(jnp.bfloat16)
        for k, g in zip(kept, got)
    ]


def flip(value, bit):
    count = lax.axis_size("tp")
    return lax.ppermute(value, "tp", [(i, i ^ bit) for i in range(count)])


def gather_columns(value):
    index = lax.axis_index("tp")
    bit = lax.axis_size("tp") // 2
    pieces = [value]
    while bit:
        others = [flip(piece, bit) for piece in pieces]
        high = (index // bit) % 2 == 1
        merged = []
        for piece, other in zip(pieces, others):
            merged += [jnp.where(high, other, piece), jnp.where(high, piece, other)]
        pieces = merged
        bit //= 2
    return jnp.concatenate(pieces, axis=1)


def send_down(down_master, rounds):
    n_fs, n_tp = lax.axis_size("fs"), lax.axis_size("tp")
    ratio = n_fs // n_tp
    mine = (lax.axis_index("fs") % ratio) * n_tp + lax.axis_index("tp")
    blocks = []
    for j in rounds:
        pairs = []
        for fs in range(n_fs):
            for tp in range(n_tp):
                expert = ((fs % ratio) * n_tp + tp) ^ j
                pairs.append((fs * n_tp + tp, expert * n_tp + fs // ratio))
        block = lax.dynamic_index_in_dim(down_master, mine ^ j, 0, keepdims=False).astype(jnp.bfloat16)
        blocks.append(lax.ppermute(block, ("fs", "tp"), pairs))
    return blocks


def collect_down(blocks):
    s = lax.axis_index("fs")
    out = jnp.zeros((len(blocks),) + blocks[0].shape, blocks[0].dtype)
    for j, block in enumerate(blocks):
        out = lax.dynamic_update_slice(out, block[None], (s ^ j, 0, 0))
    return out


def body(tokens, routes, route_weight, norm_gain, gate_master, up_master, down_master):
    rows_local = tokens.shape[0]
    model_width = tokens.shape[1]
    experts = gate_master.shape[0]
    n_tp = lax.axis_size("tp")
    n_fs = lax.axis_size("fs")
    column_count = model_width // n_tp
    tp = lax.axis_index("tp")

    row_gain = norm_gain[None, :, None]
    blocks = send_down(down_master, range(n_fs))
    gate_cast = (row_gain * gate_master).astype(jnp.bfloat16)
    gate_cast, up_master = lax.optimization_barrier((gate_cast, up_master))
    gate_serve = lax.all_to_all(gate_cast, "fs", split_axis=0, concat_axis=1, tiled=True)

    values = tokens.astype(jnp.float32)
    scale = lax.rsqrt(jnp.mean(values * values, axis=-1, keepdims=True) + 1e-06)
    share = lax.dynamic_slice_in_dim(tokens, tp * column_count, column_count, 1)
    normed = (share.astype(jnp.float32) * scale).astype(jnp.bfloat16)
    chosen = routes.reshape(-1)
    one_hot = (chosen[:, None] == jnp.arange(experts, dtype=jnp.int32)[None, :]).astype(jnp.int32)
    earlier = jnp.cumsum(one_hot, axis=0) - one_hot
    position = jnp.sum(earlier * one_hot, axis=1)
    slots = (chosen * CAP + position).reshape(rows_local, 2)
    first, second = slots[:, 0], slots[:, 1]
    slot_ids = jnp.arange(experts * CAP, dtype=jnp.int32)
    picks = ((first[None, :] == slot_ids[:, None]) | (second[None, :] == slot_ids[:, None])).astype(jnp.bfloat16)
    outgoing = jnp.dot(picks, normed, preferred_element_type=jnp.float32).astype(jnp.bfloat16)
    outgoing = outgoing.reshape(experts, CAP, column_count)
    outgoing, gate_serve = lax.optimization_barrier((outgoing, gate_serve))
    arrived = lax.all_to_all(outgoing, "fs", split_axis=0, concat_axis=0, tiled=True)
    up_cast = (row_gain * up_master).astype(jnp.bfloat16)
    up_cast, arrived = lax.optimization_barrier((up_cast, arrived))
    up_serve = lax.all_to_all(up_cast, "fs", split_axis=0, concat_axis=1, tiled=True)
    incoming = gather_columns(arrived.reshape(-1, column_count))

    gate_matrix = settled(gate_serve[0])
    up_matrix = settled(up_serve[0])
    gate_pre = jnp.dot(incoming, gate_matrix, preferred_element_type=jnp.float32)
    up_pre = jnp.dot(incoming, up_serve[0], preferred_element_type=jnp.float32)
    hidden = (jax.nn.silu(gate_pre) * up_pre).astype(jnp.bfloat16)

    piece = column_count // CHUNKS
    stored = collect_down(blocks)
    part_rows = stored.shape[1]
    ratio = n_fs // n_tp
    units = ratio * part_rows
    pairs = stored.reshape(ratio, n_tp // 2, 2, part_rows, column_count)

    def joined(part):
        return part.transpose(0, 2, 1, 3).reshape(units, -1)

    down_matrix = joined(stored.reshape(ratio, n_tp, part_rows, column_count))
    core = tp % 2
    far = joined(lax.dynamic_index_in_dim(pairs, 1 - core, 2, keepdims=False))
    near = joined(lax.dynamic_index_in_dim(pairs, core, 2, keepdims=False))
    far_part = jnp.dot(hidden, far, preferred_element_type=jnp.float32).astype(jnp.bfloat16)
    other = flip(far_part, 1)
    near_part = jnp.dot(hidden, near, preferred_element_type=jnp.float32).astype(jnp.bfloat16)
    total = (near_part.astype(jnp.float32) + other.astype(jnp.float32)).astype(jnp.bfloat16)
    owners, bit = n_tp // 2, n_tp // 2
    totals = [
        [total[:, o * column_count + c * piece : o * column_count + (c + 1) * piece] for o in range(owners)]
        for c in range(CHUNKS)
    ]
    received = {}
    while owners > 1:
        high = (tp // bit) % 2 == 1
        half = owners // 2
        for c in range(CHUNKS):
            low_part, high_part = totals[c][:half], totals[c][half:]
            kept = [jnp.where(high, h, l) for l, h in zip(low_part, high_part)]
            sent = [jnp.where(high, l, h) for l, h in zip(low_part, high_part)]
            got = [flip(x, bit) for x in sent]
            received[c] = (kept, got)
        if half > 1:
            totals = [added(*received[c]) for c in range(CHUNKS)]
        owners, bit = half, bit // 2
    outputs = []
    for c in range(CHUNKS):
        kept, got = received[c]
        if c:
            got, outputs[-1], up_matrix = lax.optimization_barrier((got, outputs[-1], up_matrix))
        total = added(kept, got)[0]
        total = total.reshape(n_fs, CAP, piece)
        returned = lax.all_to_all(total, "fs", split_axis=0, concat_axis=0, tiled=True)
        returned = returned.reshape(experts * CAP, piece)
        pick_first = (first[:, None] == slot_ids[None, :]).astype(jnp.bfloat16)
        pick_second = (second[:, None] == slot_ids[None, :]).astype(jnp.bfloat16)
        outputs.append(returned)
    columns = []
    for returned in outputs:
        one = jnp.dot(pick_first, returned, preferred_element_type=jnp.float32)
        two = jnp.dot(pick_second, returned, preferred_element_type=jnp.float32)
        columns.append(one * route_weight[:, :1] + two * route_weight[:, 1:])
    combined = jnp.concatenate(columns, axis=1).astype(jnp.bfloat16)
    return (gate_matrix[None], up_matrix[None], down_matrix[None], combined)


def solution(mesh):
    placed = (
        P("fs", None),
        P("fs", None),
        P("fs", None),
        P("fs"),
        P(None, "fs", "tp"),
        P(None, "fs", "tp"),
        P(None, "fs", "tp"),
    )

    return jax.shard_map(
        body,
        mesh=mesh,
        in_specs=placed,
        out_specs=(P("fs", None, "tp"), P("fs", None, "tp"), P("fs", "tp", None), P("fs", "tp")),
        check_vma=False,
    )
```
